32 devices in a mesh: sp: 8 (over z, y), tp: 4 (over x, core).
Axes of the slice: x: 2, y: 2, z: 4, core: 2. Of those that a mesh axis runs over, the one named last changes fastest.
Arguments:
- block_input: bfloat16 [18, 256, 2048], P(None, 'sp', 'tp'), may hold values from -6 to 6
- proj_weight: bfloat16 [2048, 2048], P(None, 'tp'), may hold values from -0.125 to 0.125
- branch_weight: bfloat16 [2048, 2048], P(None, 'tp'), may hold values from -0.125 to 0.125
- decay_gate: bfloat16 [2, 16, 128, 128], P(None, 'tp'), may hold values from -0.5 to 0.5
- input_gate: bfloat16 [2, 16, 128, 128], P(None, 'tp'), may hold values from -0.5 to 0.5
- conv_taps: bfloat16 [4, 2048], P(None, 'tp'), may hold values from -3 to 3
- decay_param: float32 [2, 2048], P(None, 'tp'), may hold values from 0 to 20, as said below
- out_cotangent: bfloat16 [18, 256, 2048], P(None, 'sp', 'tp'), may hold values from -6 to 6
Outputs:
- grad_stream: bfloat16 [18, 256, 2048], P(None, 'sp', 'tp')
- grad_branch: bfloat16 [18, 256, 2048], P(None, 'sp', 'tp')
- grad_proj: bfloat16 [2048, 2048], P('sp', 'tp')
The draws below stay inside these ranges and needn't reach their ends.
Inputs may be any that keep to these rules, and one draw needn't show every extreme that they name: softplus(-decay_param) lies between 0.02 / 256 and 0.5 / 256 for every direction and channel, so that a state keeps between about exp(-4) and exp(-0.08) of itself over a whole sequence; hence decay_param is positive and below 20.
All inputs are finite; a program needn't handle non-finite values.
Results may differ from the reference program's by a relative error of at most 0.0045.
Values may be sent and summed in bfloat16 or wider, within the bound.
A program may use at most 128 MiB of HBM per device.

```python
import math
import jax
import jax.numpy as jnp
from jax import lax

D = 2048
HEADS = 16
BLOCK = 128
BATCH = 18
TOKENS = 256


def draw_decay_param(key, part):
    layout = (2, D)
    spread = jax.random.uniform(key, layout, jnp.float32, math.log(0.02), math.log(0.5))
    decay_rate = jnp.exp(spread)
    decay_rate = decay_rate / TOKENS
    return -jnp.log(jnp.expm1(decay_rate))


def strengthened(entries, key, source, target, shards_of, factor):
    def block_of(dim):
        return (jnp.arange(entries.shape[dim]) // (entries.shape[dim] // shards_of)).reshape((-1,) + (1,) * (entries.ndim - 1 - dim))

    first = jax.random.permutation(key, shards_of)[block_of(target)]
    other_side = (block_of(target) + shards_of // 2) % shards_of
    return jnp.where((block_of(source) == first) | (block_of(source) == other_side), factor * entries, entries)


def levels(own_key, dims, shards, least, largest):
    factor_of = 1.0
    for axis_at, blocks in shards:
        draws = jax.random.uniform(jax.random.fold_in(jax.random.fold_in(own_key, 6), axis_at), (blocks,), jnp.float32, least / len(shards), largest / len(shards))
        factor_of = factor_of * jnp.repeat(jnp.exp(draws), dims[axis_at] // blocks).reshape((-1,) + (1,) * (len(dims) - 1 - axis_at))
    return factor_of


def gaussian(stream_key, extent, scale, reach, cuts=(), held_as=jnp.bfloat16):
    array = jax.random.normal(stream_key, extent, jnp.float32) * scale
    if len(cuts) > 0:
        array = levels(stream_key, extent, cuts, -0.22, 0.18) * array
    return jnp.clip(array, min=-reach, max=reach).astype(held_as)


def heavy_noise(stream_key, shape, deviation, most, split, heavy, dtype=jnp.bfloat16):
    result = deviation * jax.random.normal(stream_key, shape, jnp.float32)
    if split:
        result = result * levels(stream_key, shape, split, -0.22, 0.18)
    return jnp.clip(strengthened(result, jax.random.fold_in(stream_key, 3), *heavy), -most, most).astype(dtype)


def setup_inputs(seed: int = 0) -> dict:
    seeds = jax.random.split(jax.random.key(seed), 9)
    return {
        "block_input": heavy_noise(seeds[0], (BATCH, TOKENS, D), 1.0, 6.0, ((1, 8), (2, 4)), (1, 2, 8, 2.0)),
        "proj_weight": gaussian(seeds[1], (D, D), D ** -0.5, 0.125, ((1, 4),)),
        "branch_weight": gaussian(seeds[2], (D, D), D ** -0.5, 0.125, ((1, 4),)),
        "decay_gate": gaussian(seeds[3], (2, HEADS, BLOCK, BLOCK), BLOCK ** -0.5, 0.5, ((1, 4),)),
        "input_gate": gaussian(seeds[4], (2, HEADS, BLOCK, BLOCK), BLOCK ** -0.5, 0.5, ((1, 4),)),
        "conv_taps": gaussian(seeds[5], (4, D), 4 ** -0.5, 3.0, ((1, 4),)),
        "decay_param": draw_decay_param(jax.random.fold_in(seeds[8], 71), 0),
        "out_cotangent": gaussian(seeds[7], (BATCH, TOKENS, D), 1.0, 6.0, ((1, 8), (2, 4))),
    }


gate_scale = 8.0

def compose(former, latter):
    return (former[0] * latter[0], latter[0] * former[1] + latter[1])

def smooth(values):
    return jax.nn.gelu(values, approximate=True)

def head_map(values, weight):
    channels = values.shape[-1]
    head_count = weight.shape[1]
    by_head = values.reshape(values.shape[0], head_count, channels // head_count)
    mapped = jnp.einsum('thi,dhij->dthj', by_head, weight.astype(jnp.float32), precision=lax.Precision.HIGHEST)
    return mapped.reshape(weight.shape[0], values.shape[0], channels)

def recurrence(conv_wide, branch_wide, decay_gate, input_gate, decay_param):
    recur_gate = jax.nn.sigmoid(head_map(conv_wide, decay_gate))
    opening = jax.nn.sigmoid(head_map(conv_wide, input_gate))
    decay_rate = jax.nn.softplus(-decay_param)[:, None, :]
    log_decay = -gate_scale * recur_gate * decay_rate
    decays = jnp.exp(log_decay)
    factor = jnp.sqrt(-jnp.expm1(2.0 * log_decay))
    pushed = conv_wide * opening * factor
    states = lax.associative_scan(compose, (decays[0], pushed[0]), axis=0)[1]
    back_states = lax.associative_scan(compose, (decays[1], pushed[1]), axis=0, reverse=True)[1]
    return smooth(branch_wide) * (states + back_states)

def convolve(stream_wide, kernel):
    length = stream_wide.shape[0]
    padded = jnp.pad(stream_wide, ((1, 2), (0, 0)))
    summed = padded[0:length] * kernel[0]
    for offset in range(1, 4):
        summed = summed + padded[offset:offset + length] * kernel[offset]
    return summed

def convolve_back(gradient, kernel):
    length = gradient.shape[0]
    padded = jnp.pad(gradient, ((2, 1), (0, 0)))
    summed = padded[3:3 + length] * kernel[0]
    for offset in range(1, 4):
        summed = summed + padded[3 - offset:3 - offset + length] * kernel[offset]
    return summed

def reference(block_input, proj_weight, branch_weight, decay_gate, input_gate, conv_taps, decay_param, out_cotangent):
    kernel = conv_taps.astype(jnp.float32)

    def forward(conv_wide, branch_wide):
        return recurrence(conv_wide, branch_wide, decay_gate, input_gate, decay_param)

    def one_sequence(pieces):
        inputs, cotangent = pieces
        stream = jnp.dot(inputs, proj_weight, preferred_element_type=jnp.float32).astype(jnp.bfloat16)
        branch = jnp.dot(inputs, branch_weight, preferred_element_type=jnp.float32).astype(jnp.bfloat16)
        stream_wide = lax.optimization_barrier(stream).astype(jnp.float32)
        branch_wide = lax.optimization_barrier(branch).astype(jnp.float32)
        conv_out = convolve(stream_wide, kernel).astype(jnp.bfloat16)
        conv_wide = lax.optimization_barrier(conv_out).astype(jnp.float32)
        mixed_out, pullback = jax.vjp(forward, conv_wide, branch_wide)
        conv_grad, branch_grad = pullback(cotangent.astype(jnp.float32))
        stream_grad = convolve_back(conv_grad, kernel).astype(jnp.bfloat16)
        return (stream_grad, branch_grad.astype(jnp.bfloat16))
    grad_stream, grad_branch = lax.map(one_sequence, (block_input, out_cotangent))
    flat_input = block_input.reshape(-1, block_input.shape[-1])
    flat_grad = grad_stream.reshape(-1, grad_stream.shape[-1])
    grad_proj = jnp.dot(flat_input.T, flat_grad, preferred_element_type=jnp.float32).astype(jnp.bfloat16)
    return (grad_stream, grad_branch, grad_proj)
```

```python
import functools

import jax
import jax.numpy as jnp
from jax import lax
from jax.experimental import pallas as pl
from jax.experimental.pallas import tpu as pltpu
from jax.sharding import PartitionSpec as P

GATE_SCALE = 8.0
GELU_C = 0.7978845608028654
GELU_A = 0.044715
F32 = jnp.float32
BF16 = jnp.bfloat16


def up8(value):
    return (value + 7) // 8 * 8


def group(tokens):
    return next(size for size in (4, 2, 1) if tokens % size == 0)


def spread(source_ref, target_ref, batch, tokens, lanes, first):
    step = up8(batch)
    for b in range(batch):
        rows = source_ref[b * tokens : (b + 1) * tokens, lanes].astype(F32)
        target_ref[pl.ds(first * step + b, tokens, stride=step), :] = rows


def decay_parts(recur, rate):
    log_decay = rate * recur
    u = -2.0 * log_decay
    lost = u * (1.0 - u * (0.5 - u * (1.0 / 6.0 - u * (1.0 / 24.0))))
    inverse = lax.rsqrt(lost)
    return jnp.exp(log_decay), lost * inverse, inverse


def local_kernel(
    batch, stream_ref, halo_ref, branch_ref, cot_ref, gate_ref, taps_ref, rate_ref,
    sum_ref, g_ref, recur_ref, open_ref, sg_ref, cg_ref,
    padded, branch_t, cot_t, pre, decay, pushed,
):
    tokens = stream_ref.shape[0] // batch
    step = up8(batch)
    width = stream_ref.shape[1]
    every = slice(None)
    padded[...] = jnp.zeros_like(padded)
    branch_t[...] = jnp.zeros_like(branch_t)
    cot_t[...] = jnp.zeros_like(cot_t)
    padded[0:step] = halo_ref[0:step]
    padded[(tokens + 1) * step : (tokens + 3) * step] = halo_ref[step : 3 * step]
    spread(stream_ref, padded, batch, tokens, every, 1)
    spread(branch_ref, branch_t, batch, tokens, every, 0)
    spread(cot_ref, cot_t, batch, tokens, every, 0)
    per = group(tokens) * step
    laps = tokens // group(tokens)
    taps = taps_ref[...]

    def convolve(lap, carry):
        base = pl.multiple_of(lap * per, per)
        total = padded[pl.ds(base, per)] * taps[0:1]
        for j in range(1, 4):
            total = total + padded[pl.ds(base + j * step, per)] * taps[j : j + 1]
        g_ref[0, pl.ds(base, per)] = total.astype(BF16)
        return carry

    lax.fori_loop(0, laps, convolve, 0)
    pre[...] = jnp.dot(g_ref[0], gate_ref[0], preferred_element_type=F32)

    def gates(lap, carry):
        base = pl.multiple_of(lap * per, per)
        rows = pl.ds(base, per)
        g = g_ref[0, rows].astype(F32)
        for e in range(2):
            recur = jax.nn.sigmoid(pre[rows, 2 * e * width : (2 * e + 1) * width])
            opening = jax.nn.sigmoid(pre[rows, (2 * e + 1) * width : (2 * e + 2) * width])
            d, factor, _ = decay_parts(recur, rate_ref[e : e + 1])
            decay[e, rows] = d
            pushed[e, rows] = g * opening * factor
            recur_ref[e, 0, rows] = recur
            open_ref[e, 0, rows] = opening
        v = branch_t[rows]
        ct = cot_t[rows]
        th = jnp.tanh(GELU_C * (v + GELU_A * (v * v * v)))
        sg_ref[0, rows] = ct * (0.5 * v * (1.0 + th))
        slope = GELU_C * (1.0 + 3.0 * GELU_A * (v * v))
        cg_ref[0, rows] = ct * (0.5 * (1.0 + th) + 0.5 * v * (1.0 - th * th) * slope)
        return carry

    lax.fori_loop(0, laps, gates, 0)

    def scan(t, carry):
        a0, a1, s, b, early, late = carry
        up = pl.ds(pl.multiple_of(t * step, step), step)
        down = pl.ds(pl.multiple_of((tokens - 1 - t) * step, step), step)
        d0, d1, e0, e1 = decay[0, up], decay[1, up], decay[0, down], decay[1, down]
        return (
            a0 * d0,
            a1 * d1,
            d0 * s + pushed[0, up],
            e1 * b + pushed[1, down],
            d1 * (sg_ref[0, up] + early),
            e0 * (sg_ref[0, down] + late),
        )

    one = jnp.ones((step, width), F32)
    zero = jnp.zeros((step, width), F32)
    ends = lax.fori_loop(0, tokens, scan, (one, one, zero, zero, zero, zero))
    for i, part in enumerate(ends):
        sum_ref[i] = part


def seeded_kernel(
    batch, sums_ref, g_ref, recur_ref, open_ref, sg_ref, cg_ref, back_ref, rate_ref,
    gb_ref, grad_ref,
    decay, pushed, prev, push, mapped, recurrent,
):
    me = lax.axis_index("sp")
    count = sums_ref.shape[0]
    step = up8(batch)
    tokens = g_ref.shape[1] // step
    width = g_ref.shape[2]
    per = group(tokens) * step
    laps = tokens // group(tokens)
    zero = jnp.zeros((step, width), F32)
    s = b = early = late = zero
    for i in range(count):
        before = i < me
        a0, a1 = sums_ref[i, 0], sums_ref[i, 1]
        s = jnp.where(before, a0 * s + sums_ref[i, 2], s)
        early = jnp.where(before, a1 * early + sums_ref[i, 4], early)
        k = count - 1 - i
        after = k > me
        a0, a1 = sums_ref[k, 0], sums_ref[k, 1]
        b = jnp.where(after, a1 * b + sums_ref[k, 3], b)
        late = jnp.where(after, a0 * late + sums_ref[k, 5], late)

    def parts(lap, carry):
        rows = pl.ds(pl.multiple_of(lap * per, per), per)
        g = g_ref[0, rows].astype(F32)
        for e in range(2):
            d, factor, _ = decay_parts(recur_ref[e, 0, rows], rate_ref[e : e + 1])
            decay[e, rows] = d
            pushed[e, rows] = g * open_ref[e, 0, rows] * factor
        return carry

    lax.fori_loop(0, laps, parts, 0)

    def scan(t, carry):
        s, b, early, late = carry
        up = pl.ds(pl.multiple_of(t * step, step), step)
        down = pl.ds(pl.multiple_of((tokens - 1 - t) * step, step), step)
        prev[0, up] = s
        prev[1, down] = b
        ahead = sg_ref[0, down] + late
        behind = sg_ref[0, up] + early
        push[0, down] = ahead
        push[1, up] = behind
        return (
            decay[0, up] * s + pushed[0, up],
            decay[1, down] * b + pushed[1, down],
            decay[1, up] * behind,
            decay[0, down] * ahead,
        )

    lax.fori_loop(0, tokens, scan, (s, b, early, late))

    def gradients(lap, carry):
        rows = pl.ds(pl.multiple_of(lap * per, per), per)
        g = g_ref[0, rows].astype(F32)
        states = jnp.zeros((per, width), F32)
        direct = jnp.zeros((per, width), F32)
        for e in range(2):
            recur, opening = recur_ref[e, 0, rows], open_ref[e, 0, rows]
            rate = rate_ref[e : e + 1]
            d, factor, inverse = decay_parts(recur, rate)
            before, grad = prev[e, rows] * d, push[e, rows]
            gated = g * opening
            states = states + (before + gated * factor)
            through = grad * opening * factor
            direct = direct + through
            log_grad = grad * (before - gated * (d * d) * inverse)
            recur_pre = log_grad * rate * (recur * (1.0 - recur))
            open_pre = through * g * (1.0 - opening)
            mapped[rows, 2 * e * width : (2 * e + 1) * width] = recur_pre.astype(BF16)
            mapped[rows, (2 * e + 1) * width : (2 * e + 2) * width] = open_pre.astype(BF16)
        recurrent[rows] = states * cg_ref[0, rows]
        grad_ref[0, rows] = direct
        return carry

    lax.fori_loop(0, laps, gradients, 0)
    grad_ref[0] = grad_ref[0] + jnp.dot(mapped[...], back_ref[0], preferred_element_type=F32)
    for i in range(batch):
        gb_ref[i * tokens : (i + 1) * tokens] = recurrent[pl.ds(i, tokens, stride=step), :].astype(BF16)


def stream_grad_kernel(batch, grad_ref, halo_ref, taps_ref, out_ref, padded, result):
    step = up8(batch)
    tokens = grad_ref.shape[1] // step
    per = group(tokens) * step
    laps = tokens // group(tokens)
    taps = taps_ref[...]
    padded[0 : 2 * step] = halo_ref[0 : 2 * step]
    padded[(tokens + 2) * step : (tokens + 3) * step] = halo_ref[2 * step : 3 * step]
    padded[2 * step : (tokens + 2) * step] = grad_ref[0]

    def convolve(lap, carry):
        base = pl.multiple_of(lap * per, per)
        total = padded[pl.ds(base + 3 * step, per)] * taps[0:1]
        for j in range(1, 4):
            total = total + padded[pl.ds(base + (3 - j) * step, per)] * taps[j : j + 1]
        result[pl.ds(base, per)] = total
        return carry

    lax.fori_loop(0, laps, convolve, 0)
    for i in range(batch):
        out_ref[i * tokens : (i + 1) * tokens] = result[pl.ds(i, tokens, stride=step), :].astype(BF16)


def shift(values, axis, onward):
    count = lax.axis_size(axis)
    pairs = [(i, i + 1) if onward else (i + 1, i) for i in range(count - 1)]
    return lax.ppermute(values, axis, pairs)


def shards(
    block_input, proj_weight, branch_weight, decay_gate, input_gate, conv_taps, decay_param, out_cotangent,
):
    batch, tokens, _ = block_input.shape
    heads, width = decay_gate.shape[1], decay_gate.shape[2]
    channels = heads * width
    step = up8(batch)
    rows, rows_t = batch * tokens, tokens * step
    gathered = lax.all_gather(block_input, "tp", axis=2, tiled=True).reshape(rows, -1)
    stream = jnp.dot(gathered, proj_weight, preferred_element_type=F32).astype(BF16)
    branch = jnp.dot(gathered, branch_weight, preferred_element_type=F32).astype(BF16)
    taps = conv_taps.astype(F32)
    rate = -GATE_SCALE * jax.nn.softplus(-decay_param)
    gate = jnp.concatenate([decay_gate[0], input_gate[0], decay_gate[1], input_gate[1]], axis=2)
    back = jnp.swapaxes(gate, 1, 2)

    by_token = stream.reshape(batch, tokens, channels)
    tail = shift(by_token[:, -1:], "sp", True)
    head = shift(by_token[:, :2], "sp", False)
    halo = jnp.concatenate([tail, head], axis=1).astype(F32)
    halo = jnp.pad(jnp.swapaxes(halo, 0, 1), ((0, 0), (0, step - batch), (0, 0))).reshape(3 * step, channels)

    def column(count):
        return pl.BlockSpec((count, width), lambda h: (0, h))

    def per_head(count, size):
        return pl.BlockSpec((1, count, size), lambda h: (h, 0, 0))

    def pair(count):
        return pl.BlockSpec((2, 1, count, width), lambda h: (0, h, 0, 0))

    def scratch(*shape):
        return pltpu.VMEM(shape + (width,), F32)

    def of(dtype, *shape):
        return jax.ShapeDtypeStruct(shape, dtype)

    params = pltpu.CompilerParams(vmem_limit_bytes=48 * 1024 * 1024)
    sums, g, recur, opening, sg, cg = pl.pallas_call(
        functools.partial(local_kernel, batch),
        grid=(heads,),
        in_specs=[column(rows), column(3 * step), column(rows), column(rows), per_head(width, 4 * width), column(4), column(2)],
        out_specs=[
            pl.BlockSpec((6, step, width), lambda h: (0, 0, h)),
            per_head(rows_t, width), pair(rows_t), pair(rows_t), per_head(rows_t, width), per_head(rows_t, width),
        ],
        out_shape=[
            of(F32, 6, step, channels), of(BF16, heads, rows_t, width), of(F32, 2, heads, rows_t, width),
            of(F32, 2, heads, rows_t, width), of(F32, heads, rows_t, width), of(F32, heads, rows_t, width),
        ],
        scratch_shapes=[
            scratch((tokens + 3) * step), scratch(rows_t), scratch(rows_t),
            pltpu.VMEM((rows_t, 4 * width), F32), scratch(2, rows_t), scratch(2, rows_t),
        ],
        compiler_params=params,
        name="local_scan",
    )(stream, halo, branch, out_cotangent.reshape(rows, channels), gate, taps, rate)

    sums = lax.all_gather(sums, "sp")
    count = sums.shape[0]
    grad_branch, conv_grad = pl.pallas_call(
        functools.partial(seeded_kernel, batch),
        grid=(heads,),
        in_specs=[
            pl.BlockSpec((count, 6, step, width), lambda h: (0, 0, 0, h)),
            per_head(rows_t, width), pair(rows_t), pair(rows_t), per_head(rows_t, width), per_head(rows_t, width),
            per_head(4 * width, width), column(2),
        ],
        out_specs=[column(rows), per_head(rows_t, width)],
        out_shape=[of(BF16, rows, channels), of(F32, heads, rows_t, width)],
        scratch_shapes=[
            scratch(2, rows_t), scratch(2, rows_t), scratch(2, rows_t), scratch(2, rows_t),
            pltpu.VMEM((rows_t, 4 * width), BF16), scratch(rows_t),
        ],
        compiler_params=params,
        name="seeded_scan",
    )(sums, g, recur, opening, sg, cg, back, rate)

    grad_tail = shift(conv_grad[:, rows_t - 2 * step :], "sp", True)
    grad_head = shift(conv_grad[:, :step], "sp", False)
    grad_halo = jnp.swapaxes(jnp.concatenate([grad_tail, grad_head], axis=1), 0, 1).reshape(3 * step, channels)
    grad_stream = pl.pallas_call(
        functools.partial(stream_grad_kernel, batch),
        grid=(heads,),
        in_specs=[per_head(rows_t, width), column(3 * step), column(4)],
        out_specs=column(rows),
        out_shape=of(BF16, rows, channels),
        scratch_shapes=[scratch((tokens + 3) * step), scratch(rows_t)],
        compiler_params=params,
        name="stream_grad",
    )(conv_grad, grad_halo, taps)
    portion = lax.dot_general(
        gathered, grad_stream, (((0,), (0,)), ((), ())), preferred_element_type=F32
    )
    grad_proj = lax.psum_scatter(portion, "sp", scatter_dimension=0, tiled=True).astype(BF16)
    shape = (batch, tokens, channels)
    return (grad_stream.reshape(shape), grad_branch.reshape(shape), grad_proj)


def solution(mesh):
    return jax.shard_map(
        shards,
        mesh=mesh,
        in_specs=(
            P(None, "sp", "tp"),
            P(None, "tp"),
            P(None, "tp"),
            P(None, "tp", None, None),
            P(None, "tp", None, None),
            P(None, "tp"),
            P(None, "tp"),
            P(None, "sp", "tp"),
        ),
        out_specs=(P(None, "sp", "tp"), P(None, "sp", "tp"), P("sp", "tp")),
        check_vma=False,
    )
```
